32 devices in a mesh: dp: 4 (over y, x), kv: 4 (over z), tp: 2 (over core).
Axes of the slice: x: 2, y: 2, z: 4, core: 2. Of those that a mesh axis runs over, the one named last changes fastest.
Arguments:
- tokens: bfloat16 [192, 2048], P(('dp', 'tp'), 'kv'), may hold values from -8 to 8
- mix_gain: float32 [2048], replicated, may hold values from 0.1 to 1.9
- w_gate: bfloat16 [2048, 4096], P(None, 'kv'), may hold values from -0.125 to 0.125
- w_value: bfloat16 [2048, 4096], P(None, 'kv'), may hold values from -0.125 to 0.125
- w_maps: bfloat16 [2048, 16384], P(None, 'kv'), may hold values from -0.125 to 0.125
- w_step: bfloat16 [2048, 64], replicated, may hold values from -0.125 to 0.125
- conv_value: float32 [4, 4096], P(None, 'kv'), may hold values from -0.5 to 0.5
- conv_maps: float32 [4, 16384], P(None, 'kv'), may hold values from -0.5 to 0.5
- past_value: bfloat16 [192, 3, 4096], P(('dp', 'tp'), None, 'kv'), may hold values from -6 to 6
- past_maps: bfloat16 [192, 3, 16384], P(('dp', 'tp'), None, 'kv'), may hold values from -6 to 6
- step_bias: float32 [64], P('kv'), may hold values from -3 to 0
- decay_log: float32 [64], P('kv'), may hold values from 0 to 2.77
- skip_gain: float32 [64], P('kv'), may hold values from 0.1 to 1.9
- head_gain: float32 [4096], P('kv'), may hold values from 0.1 to 1.9
- state: float32 [192, 64, 64, 128], P(('dp', 'tp'), 'kv'), may hold values from -2 to 2
- w_out: bfloat16 [4096, 2048], P('kv'), may hold values from -0.125 to 0.125
- mlp_gain: float32 [2048], replicated, may hold values from 0.1 to 1.9
- w_up: bfloat16 [2048, 8192], P(None, 'kv'), may hold values from -0.125 to 0.125
- w_down: bfloat16 [8192, 2048], P('kv'), may hold values from -0.09375 to 0.09375
Outputs:
- layer_out: bfloat16 [192, 2048], P(('dp', 'tp'), 'kv')
- state_next: float32 [192, 64, 64, 128], P(('dp', 'tp'), 'kv')
- value_tail: bfloat16 [192, 3, 4096], P(('dp', 'tp'), None, 'kv')
- maps_tail: bfloat16 [192, 3, 16384], P(('dp', 'tp'), None, 'kv')
The draws below stay inside these ranges and needn't reach their ends.
All inputs are finite; a program needn't handle non-finite values.
Results may differ from the reference program's by a relative error of at most 0.0081.
Values may be sent and summed in bfloat16 or wider, within the bound.
A program may use at most 128 MiB of HBM per device.

```python
import jax
import jax.numpy as jnp
from jax import lax

D = 2048
HEADS = 64
HEAD_DIM = 64
STATE = 128
GROUPS = 64
KERNEL = 4
FF = 8192
INNER = 4096
MAPS = 16384
BATCH = 192


def draw_tokens(key, part):
    streams = jax.random.split(jax.random.fold_in(key, 17), 4)
    columns = jnp.arange(D, dtype=jnp.float32)
    spread = jnp.exp(jax.random.uniform(streams[0], (D,), jnp.float32) * jnp.log(10.0))
    col_scale = spread * (1.0 + 3.0 * columns / D)
    col_scale = col_scale / jnp.sqrt(jnp.mean(col_scale * col_scale))
    noise_part = jax.random.normal(streams[1], (BATCH, D), jnp.float32)
    row_scale = jnp.exp(jax.random.uniform(streams[3], (BATCH, 1), jnp.float32, -0.35, 0.35))
    return jnp.clip(noise_part * col_scale[None, :] * row_scale, -8.0, 8.0).astype(jnp.bfloat16)


def with_spikes(result, stream_key, source, target, shards_of, factor):
    def block_of(position):
        return (jnp.arange(result.shape[position]) // (result.shape[position] // shards_of)).reshape((-1,) + (1,) * (result.ndim - 1 - position))

    near = jax.random.permutation(stream_key, shards_of)[block_of(target)]
    far = (block_of(target) + shards_of // 2) % shards_of
    return jnp.where((block_of(source) == near) | (block_of(source) == far), factor * result, result)


def block_levels(own_key, extent, cuts, least, largest):
    def one(position, shards_of):
        heights = jax.random.uniform(jax.random.fold_in(jax.random.fold_in(own_key, 6), position), (shards_of,), jnp.float32, least / len(cuts), largest / len(cuts))
        return jnp.repeat(jnp.exp(heights), extent[position] // shards_of).reshape((-1,) + (1,) * (len(extent) - position - 1))

    level = one(*cuts[0])
    for cut in cuts[1:]:
        level = level * one(*cut)
    return level


def noise(own_key, shape, scale, bound, cuts=(), kind=jnp.bfloat16):
    entries = jax.random.normal(own_key, shape, jnp.float32) * scale
    if len(cuts) > 0:
        entries = block_levels(own_key, shape, cuts, -0.22, 0.18) * entries
    return jnp.clip(entries, min=-bound, max=bound).astype(kind)


def heavy_noise(own_key, shape, deviation, limit, cuts, heavy, kind=jnp.bfloat16):
    entries = deviation * jax.random.normal(own_key, shape, jnp.float32)
    if cuts:
        entries = entries * block_levels(own_key, shape, cuts, -0.22, 0.18)
    return jnp.clip(with_spikes(entries, jax.random.fold_in(own_key, 3), *heavy), -limit, limit).astype(kind)


def setup_inputs(seed: int = 0) -> dict:
    streams_of = jax.random.split(jax.random.key(seed), 20)
    return {
        "tokens": draw_tokens(jax.random.fold_in(streams_of[19], 71), 0),
        "mix_gain": jnp.clip(1.0 + 0.18 * jax.random.normal(streams_of[1], (D,), jnp.float32), 0.1, 1.9),
        "w_gate": noise(streams_of[2], (D, INNER), D ** -0.5, 0.125, ((1, 4),)),
        "w_value": noise(streams_of[3], (D, INNER), D ** -0.5, 0.125, ((1, 4),)),
        "w_maps": noise(streams_of[4], (D, MAPS), D ** -0.5, 0.125, ((1, 4),)),
        "w_step": noise(streams_of[5], (D, HEADS), D ** -0.5, 0.125),
        "conv_value": jnp.clip(jax.random.uniform(streams_of[6], (KERNEL, INNER), jnp.float32, -0.5, 0.5) * block_levels(streams_of[6], (KERNEL, INNER), ((1, 4),), -0.4, 0.0), -0.5, 0.5),
        "conv_maps": jnp.clip(jax.random.uniform(streams_of[7], (KERNEL, MAPS), jnp.float32, -0.5, 0.5) * block_levels(streams_of[7], (KERNEL, MAPS), ((1, 4),), -0.4, 0.0), -0.5, 0.5),
        "past_value": noise(streams_of[8], (BATCH, KERNEL - 1, INNER), 1.0, 6.0, ((0, 8), (2, 4))),
        "past_maps": noise(streams_of[9], (BATCH, KERNEL - 1, MAPS), 1.0, 6.0, ((0, 8), (2, 4))),
        "step_bias": jnp.clip(-3.0 + 3.0 * jax.random.uniform(streams_of[10], (HEADS,), jnp.float32) ** block_levels(streams_of[10], (HEADS,), ((0, 4),), -0.2, 0.2), -3.0, 0.0),
        "decay_log": jnp.clip(2.77 * jax.random.uniform(streams_of[11], (HEADS,), jnp.float32) ** block_levels(streams_of[11], (HEADS,), ((0, 4),), -0.2, 0.2), 0.0, 2.77),
        "skip_gain": jnp.clip(1.0 + 0.18 * jax.random.normal(streams_of[12], (HEADS,), jnp.float32), 0.1, 1.9),
        "head_gain": jnp.clip(1.0 + 0.18 * jax.random.normal(streams_of[13], (INNER,), jnp.float32), 0.1, 1.9),
        "state": noise(streams_of[14], (BATCH, HEADS, HEAD_DIM, STATE), 0.3, 2.0, ((0, 8), (1, 4)), jnp.float32),
        "w_out": heavy_noise(streams_of[15], (INNER, D), INNER ** -0.5, 0.125, ((0, 4),), (0, 1, 4, 2.0)),
        "mlp_gain": jnp.clip(1.0 + 0.18 * jax.random.normal(streams_of[16], (D,), jnp.float32), 0.1, 1.9),
        "w_up": noise(streams_of[17], (D, FF), D ** -0.5, 0.125, ((1, 4),)),
        "w_down": heavy_noise(streams_of[18], (FF, D), FF ** -0.5, 0.09375, ((0, 4),), (0, 1, 4, 2.0)),
    }


NORM_EPS = 1e-05

def rms_rows(matrix, gain_vec):
    widened = matrix.astype(jnp.float32)
    inv_scale = lax.rsqrt(lax.optimization_barrier(jnp.mean(widened * widened, axis=-1, keepdims=True)) + NORM_EPS)
    return (widened * inv_scale * gain_vec).astype(jnp.bfloat16)

def short_conv(past_rows, newest, kernel):
    window = jnp.concatenate([past_rows, newest[:, None, :]], axis=1)
    summed = lax.optimization_barrier(jnp.sum(window.astype(jnp.float32) * kernel[None], axis=1))
    return (jax.nn.silu(summed), window[:, 1:, :])

def reference(tokens, mix_gain, w_gate, w_value, w_maps, w_step, conv_value, conv_maps, past_value, past_maps, step_bias, decay_log, skip_gain, head_gain, state, w_out, mlp_gain, w_up, w_down):
    normed = rms_rows(tokens, mix_gain)
    gate_pre = jnp.dot(normed, w_gate, preferred_element_type=jnp.float32)
    step_pre = jnp.dot(normed, w_step, preferred_element_type=jnp.float32)
    value_new = jnp.dot(normed, w_value, preferred_element_type=jnp.float32).astype(jnp.bfloat16)
    maps_new = jnp.dot(normed, w_maps, preferred_element_type=jnp.float32).astype(jnp.bfloat16)
    value_act, value_tail = short_conv(past_value, value_new, conv_value)
    maps_act, maps_tail = short_conv(past_maps, maps_new, conv_maps)
    rounded = lax.optimization_barrier(maps_act.astype(jnp.bfloat16))
    grouped = rounded.astype(jnp.float32).reshape(BATCH, GROUPS, 2, STATE)
    per_group = HEADS // GROUPS
    in_map = jnp.repeat(grouped[:, :, 0], per_group, axis=1)
    out_map = jnp.repeat(grouped[:, :, 1], per_group, axis=1)
    head_values = value_act.reshape(BATCH, HEADS, HEAD_DIM)
    step_size = jax.nn.softplus(step_pre + step_bias)
    decay_rate = jnp.exp(-step_size * jnp.exp(decay_log))
    written = (step_size[:, :, None] * head_values)[:, :, :, None] * in_map[:, :, None, :]
    state_next = decay_rate[:, :, None, None] * state + written
    read_out = lax.optimization_barrier(jnp.sum(state_next * out_map[:, :, None, :], axis=-1)) + skip_gain[None, :, None] * head_values
    gated_heads = read_out * jax.nn.silu(gate_pre.reshape(BATCH, HEADS, HEAD_DIM))
    inv_scale = lax.rsqrt(lax.optimization_barrier(jnp.mean(gated_heads * gated_heads, axis=-1, keepdims=True)) + NORM_EPS)
    heads_out = (gated_heads * inv_scale * head_gain.reshape(HEADS, HEAD_DIM)).reshape(BATCH, INNER)
    heads_out = heads_out.astype(jnp.bfloat16)
    mixer_out = jnp.dot(heads_out, w_out, preferred_element_type=jnp.float32)
    hidden = lax.optimization_barrier((tokens.astype(jnp.float32) + mixer_out).astype(jnp.bfloat16))
    normed_mlp = rms_rows(hidden, mlp_gain)
    squared = jnp.square(jax.nn.relu(jnp.dot(normed_mlp, w_up, preferred_element_type=jnp.float32)))
    squared = squared.astype(jnp.bfloat16)
    layer_out = hidden.astype(jnp.float32) + jnp.dot(squared, w_down, preferred_element_type=jnp.float32)
    return (layer_out.astype(jnp.bfloat16), state_next, value_tail, maps_tail)
```

```python
import functools

import jax
import jax.numpy as jnp
from jax import lax
from jax.experimental import pallas as pl
from jax.experimental.pallas import tpu as pltpu
from jax.sharding import PartitionSpec as P

HEAD_DIM = 64
STATE = 128
MESH = pl.DeviceIdType.MESH
VMEM_LIMIT = 60 * 1024 * 1024


NORM_EPS = 1e-05
NT = (((1,), (1,)), ((), ()))


def greet(peers, me):
    barrier = pltpu.get_barrier_semaphore()
    for d in range(1, peers):
        pl.semaphore_signal(
            barrier, inc=1, device_id={"kv": lax.rem(me + d, peers)}, device_id_type=MESH
        )
    pl.semaphore_wait(barrier, peers - 1)


def push(src, dst, send_sem, recv_sem, target):
    return pltpu.make_async_remote_copy(
        src_ref=src,
        dst_ref=dst,
        send_sem=send_sem,
        recv_sem=recv_sem,
        device_id={"kv": target},
        device_id_type=MESH,
    )


def project_kernel(
    peers,
    tokens,
    gain,
    w_step,
    bias,
    decay_log,
    w_gate,
    w_value,
    w_maps,
    gate_out,
    value_out,
    maps_out,
    step_out,
    decay_out,
    slots,
    weights,
    acc,
    w_sem,
    send_sem,
    recv_sem,
):
    me = lax.axis_index("kv")
    rows, part = tokens.shape
    chunks, width = weights.shape[1], weights.shape[3]
    heads = decay_out.shape[1]
    inner = value_out.shape[1]

    def source(c):
        for ref in (w_gate, w_value, w_maps):
            n = ref.shape[1] // width
            if c < n:
                return ref, c * width
            c -= n

    for d in range(peers):
        start = pl.multiple_of(lax.rem(me + d, peers) * part, part)
        for c in range(chunks):
            ref, col = source(c)
            pltpu.make_async_copy(
                ref.at[pl.ds(start, part), pl.ds(col, width)], weights.at[d, c], w_sem.at[d, c]
            ).start()

    greet(peers, me)
    sends = []
    for d in range(1, peers):
        cp = push(
            tokens,
            slots.at[peers - d],
            send_sem.at[d],
            recv_sem.at[peers - d],
            lax.rem(me + d, peers),
        )
        cp.start()
        sends.append(cp)

    squares = jnp.zeros((rows, 1), jnp.float32)
    step_pre = jnp.zeros((rows, w_step.shape[0]), jnp.float32)
    for d in range(peers):
        start = pl.multiple_of(lax.rem(me + d, peers) * part, part)
        if d == 0:
            raw = tokens[...]
        else:
            push(tokens, slots.at[d], send_sem.at[d], recv_sem.at[d], me).wait_recv()
            raw = slots[d]
        wide = raw.astype(jnp.float32)
        squares = squares + jnp.sum(wide * wide, axis=1, keepdims=True)
        scaled = (wide * gain[:, pl.ds(start, part)]).astype(jnp.bfloat16)
        step_pre = step_pre + lax.dot_general(
            scaled, w_step[:, pl.ds(start, part)], NT, preferred_element_type=jnp.float32
        )

        def chunk(c, carry, d=d, scaled=scaled):
            pltpu.make_async_copy(
                w_gate.at[pl.ds(0, part), pl.ds(0, width)], weights.at[d, c], w_sem.at[d, c]
            ).wait()
            out = jnp.dot(scaled, weights[d, c], preferred_element_type=jnp.float32)
            acc[c] = out if d == 0 else acc[c] + out
            return carry

        lax.fori_loop(0, chunks, chunk, 0)

    inv = lax.rsqrt(squares / (peers * part) + NORM_EPS)
    for c in range(chunks):
        total = acc[c] * inv
        ref, col = source(c)
        if ref is w_gate:
            gate_out[:, pl.ds(col, width)] = total
        elif ref is w_value:
            value_out[:, pl.ds(col, width)] = total.astype(jnp.bfloat16)
        else:
            maps_out[:, pl.ds(col, width)] = total.astype(jnp.bfloat16)
    step_pre = step_pre * inv
    own = step_pre[:, :heads]
    for j in range(1, peers):
        own = jnp.where(me == j, step_pre[:, j * heads : (j + 1) * heads], own)
    own = own + bias[...]
    step = jnp.maximum(own, 0.0) + jnp.log1p(jnp.exp(-jnp.abs(own)))
    decay_out[...] = jnp.exp(-step * jnp.exp(decay_log[...]))
    lane = lax.broadcasted_iota(jnp.int32, (rows, 2 * HEAD_DIM), 1)
    for h in range(0, heads, 2):
        step_out[:, h * HEAD_DIM : (h + 2) * HEAD_DIM] = jnp.where(
            lane < HEAD_DIM, step[:, h : h + 1], step[:, h + 1 : h + 2]
        )
    for cp in sends:
        cp.wait_send()


def project(peers, tokens, mix_gain, w_step, step_bias, decay_log, w_gate, w_value, w_maps):
    rows, part = tokens.shape
    heads = step_bias.shape[0]
    inner, maps = w_value.shape[1], w_maps.shape[1]
    width = min(1024, inner)
    chunks = (2 * inner + maps) // width
    f32 = jnp.float32
    vmem = pl.BlockSpec(memory_space=pltpu.VMEM)
    hbm = pl.BlockSpec(memory_space=pl.ANY)
    return pl.pallas_call(
        functools.partial(project_kernel, peers),
        out_shape=(
            jax.ShapeDtypeStruct((rows, inner), f32),
            jax.ShapeDtypeStruct((rows, inner), jnp.bfloat16),
            jax.ShapeDtypeStruct((rows, maps), jnp.bfloat16),
            jax.ShapeDtypeStruct((rows, inner), f32),
            jax.ShapeDtypeStruct((rows, heads), f32),
        ),
        in_specs=[vmem] * 5 + [hbm] * 3,
        out_specs=(vmem,) * 5,
        scratch_shapes=[
            pltpu.VMEM((peers, rows, part), jnp.bfloat16),
            pltpu.VMEM((peers, chunks, part, width), jnp.bfloat16),
            pltpu.VMEM((chunks, rows, width), f32),
            pltpu.SemaphoreType.DMA((peers, chunks)),
            pltpu.SemaphoreType.DMA((peers,)),
            pltpu.SemaphoreType.DMA((peers,)),
        ],
        compiler_params=pltpu.CompilerParams(
            collective_id=0, has_side_effects=True, vmem_limit_bytes=VMEM_LIMIT
        ),
        name="project",
    )(
        tokens,
        mix_gain[None, :],
        w_step.T,
        step_bias[None, :],
        decay_log[None, :],
        w_gate,
        w_value,
        w_maps,
    )


def silu(x):
    return x * jax.nn.sigmoid(x)


def state_kernel(
    decay,
    skip,
    state,
    gate,
    value_new,
    maps_new,
    step,
    past_value,
    past_maps,
    conv_value,
    conv_maps,
    head_gain,
    heads_out,
    state_out,
    value_tail,
    maps_tail,
):
    i = pl.program_id(0)
    rows = state.shape[0]

    def conv(past, new, taps, tail):
        taps_n = past.shape[0]
        total = new[...].astype(jnp.float32) * taps[taps_n : taps_n + 1, :]
        for k in range(taps_n):
            row = past[k]
            total = total + row.astype(jnp.float32) * taps[k : k + 1, :]
            if k > 0:
                tail[k - 1] = row
        tail[taps_n - 1] = new[...]
        return silu(total)

    value_act = conv(past_value, value_new, conv_value, value_tail)
    maps_act = conv(past_maps, maps_new, conv_maps, maps_tail)
    maps_act = maps_act.astype(jnp.bfloat16).astype(jnp.float32)

    scaled = value_act * step[...]
    high = scaled.astype(jnp.bfloat16).astype(jnp.float32)
    both = jnp.concatenate([high, scaled - high], axis=0).T.astype(jnp.bfloat16)
    ins = []
    outs = []
    for hh in range(2):
        at = 2 * hh * STATE
        ins.append(jnp.concatenate([maps_act[:, at : at + STATE]] * 2, axis=0))
        outs.append(maps_act[:, at + STATE : at + 2 * STATE])
    readers = jnp.concatenate(outs, axis=0).astype(jnp.bfloat16)

    row = lax.broadcasted_iota(jnp.int32, (2 * rows, STATE), 0)
    lane = lax.broadcasted_iota(jnp.int32, (2 * rows, STATE), 1)
    seq = jnp.where(row >= rows, row - rows, row)
    owner = jnp.where((row >= rows) == (lane >= HEAD_DIM), seq, -1)
    read = jnp.zeros((2 * rows, 2 * HEAD_DIM), jnp.float32)
    for b in range(0, rows, 2):
        fresh = [None] * 4
        for hh in range(2):
            spread = jnp.concatenate(
                [jnp.where(seq == b + k, ins[hh], 0.0) for k in range(2)], axis=1
            ).astype(jnp.bfloat16)
            written = jnp.dot(
                both[hh * HEAD_DIM : (hh + 1) * HEAD_DIM],
                spread,
                preferred_element_type=jnp.float32,
            )
            for k in range(2):
                new = (
                    decay[b + k, 2 * i + hh] * state[b + k, hh]
                    + written[:, k * STATE : (k + 1) * STATE]
                )
                state_out[b + k, hh] = new
                fresh[2 * k + hh] = new.astype(jnp.bfloat16)
        found = lax.dot_general(
            readers, jnp.concatenate(fresh, axis=0), NT, preferred_element_type=jnp.float32
        )
        for k in range(2):
            read = read + jnp.where(
                owner == b + k, found[:, k * 2 * HEAD_DIM : (k + 1) * 2 * HEAD_DIM], 0.0
            )
    first = lane[:rows] < HEAD_DIM
    read_out = read[:rows] + read[rows:]
    read_out = read_out + jnp.where(first, skip[2 * i], skip[2 * i + 1]) * value_act
    gated = read_out * silu(gate[...])
    square = gated * gated
    low = jnp.sum(jnp.where(first, square, 0.0), axis=1, keepdims=True)
    top = jnp.sum(jnp.where(first, 0.0, square), axis=1, keepdims=True)
    inv = lax.rsqrt(jnp.where(first, low, top) / HEAD_DIM + NORM_EPS)
    heads_out[...] = (gated * inv * head_gain[...]).astype(jnp.bfloat16)


def step_state(
    decay,
    skip_gain,
    state,
    gate,
    value_new,
    maps_new,
    step,
    past_value,
    past_maps,
    conv_value,
    conv_maps,
    head_gain,
):
    rows, heads = state.shape[:2]
    smem = pl.BlockSpec(memory_space=pltpu.SMEM)
    pair = 2 * HEAD_DIM
    wide = 4 * STATE
    taps = conv_value.shape[0]
    past_v = jnp.swapaxes(past_value, 0, 1)
    past_m = jnp.swapaxes(past_maps, 0, 1)
    flat = lambda width: pl.BlockSpec((rows, width), lambda i: (0, i))
    conv_spec = lambda width: pl.BlockSpec((taps, width), lambda i: (0, i))
    past_spec = lambda width: pl.BlockSpec((taps - 1, rows, width), lambda i: (0, 0, i))
    state_spec = pl.BlockSpec((rows, 2, HEAD_DIM, STATE), lambda i: (0, i, 0, 0))
    heads_out, state_next, tail_v, tail_m = pl.pallas_call(
        state_kernel,
        grid=(heads // 2,),
        out_shape=(
            jax.ShapeDtypeStruct((rows, heads * HEAD_DIM), jnp.bfloat16),
            jax.ShapeDtypeStruct(state.shape, jnp.float32),
            jax.ShapeDtypeStruct(past_v.shape, jnp.bfloat16),
            jax.ShapeDtypeStruct(past_m.shape, jnp.bfloat16),
        ),
        in_specs=[
            smem,
            smem,
            state_spec,
            flat(pair),
            flat(pair),
            flat(wide),
            flat(pair),
            past_spec(pair),
            past_spec(wide),
            conv_spec(pair),
            conv_spec(wide),
            pl.BlockSpec((1, pair), lambda i: (0, i)),
        ],
        out_specs=(flat(pair), state_spec, past_spec(pair), past_spec(wide)),
        compiler_params=pltpu.CompilerParams(
            dimension_semantics=("arbitrary",), vmem_limit_bytes=VMEM_LIMIT
        ),
        name="step_state",
    )(
        decay,
        skip_gain,
        state,
        gate,
        value_new,
        maps_new,
        step,
        past_v,
        past_m,
        conv_value,
        conv_maps,
        head_gain[None, :],
    )
    return heads_out, state_next, jnp.swapaxes(tail_v, 0, 1), jnp.swapaxes(tail_m, 0, 1)


def mixer_kernel(
    peers,
    heads,
    tokens,
    gain,
    w_out,
    w_up,
    w_down,
    layer_out,
    out_w,
    up_w,
    down_w,
    sums_a,
    land_a,
    own_hidden,
    hidden,
    up_acc,
    squared,
    sums_b,
    land_b,
    out_sem,
    up_sem,
    down_sem,
    send_a,
    recv_a,
    send_h,
    recv_h,
    send_b,
    recv_b,
):
    me = lax.axis_index("kv")
    rows, part = tokens.shape
    n_up, width = up_w.shape[1], up_w.shape[3]

    def place(d):
        return pl.multiple_of(lax.rem(me + d, peers) * part, part)

    order = list(range(1, peers)) + [0]
    waits_out, waits_down = {}, {}
    for d in order:
        cp = pltpu.make_async_copy(w_out.at[:, pl.ds(place(d), part)], out_w.at[d], out_sem.at[d])
        cp.start()
        waits_out[d] = cp
    for d in range(peers):
        for c in range(n_up):
            pltpu.make_async_copy(
                w_up.at[pl.ds(place(d), part), pl.ds(c * width, width)],
                up_w.at[d, c],
                up_sem.at[d, c],
            ).start()
    for d in order:
        cp = pltpu.make_async_copy(
            w_down.at[:, pl.ds(place(d), part)], down_w.at[d], down_sem.at[d]
        )
        cp.start()
        waits_down[d] = cp

    greet(peers, me)
    pending = []

    def scatter(left, weights, waits, sums, land, send, recv):
        for d in order:
            waits[d].wait()
            piece = jnp.dot(left, weights[d], preferred_element_type=jnp.float32)
            if d == 0:
                total = piece
            else:
                sums[d] = piece
                cp = push(
                    sums.at[d],
                    land.at[peers - d],
                    send.at[d],
                    recv.at[peers - d],
                    lax.rem(me + d, peers),
                )
                cp.start()
                pending.append(cp)
        for d in range(1, peers):
            push(sums.at[d], land.at[d], send.at[d], recv.at[d], me).wait_recv()
            total = total + land[d]
        return total

    total = scatter(heads[...], out_w, waits_out, sums_a, land_a, send_a, recv_a)
    mine = (tokens[...].astype(jnp.float32) + total).astype(jnp.bfloat16)
    own_hidden[...] = mine
    for d in range(1, peers):
        cp = push(
            own_hidden,
            hidden.at[peers - d],
            send_h.at[d],
            recv_h.at[peers - d],
            lax.rem(me + d, peers),
        )
        cp.start()
        pending.append(cp)

    squares = jnp.zeros((rows, 1), jnp.float32)
    for d in range(peers):
        if d == 0:
            raw = mine
        else:
            push(own_hidden, hidden.at[d], send_h.at[d], recv_h.at[d], me).wait_recv()
            raw = hidden[d]
        wide = raw.astype(jnp.float32)
        squares = squares + jnp.sum(wide * wide, axis=1, keepdims=True)
        scaled = (wide * gain[:, pl.ds(place(d), part)]).astype(jnp.bfloat16)

        def chunk(c, carry, d=d, scaled=scaled):
            pltpu.make_async_copy(
                w_up.at[pl.ds(0, part), pl.ds(0, width)], up_w.at[d, c], up_sem.at[d, c]
            ).wait()
            out = jnp.dot(scaled, up_w[d, c], preferred_element_type=jnp.float32)
            up_acc[c] = out if d == 0 else up_acc[c] + out
            return carry

        lax.fori_loop(0, n_up, chunk, 0)

    inv = lax.rsqrt(squares / (peers * part) + NORM_EPS)
    for c in range(n_up):
        up = jnp.maximum(up_acc[c] * inv, 0.0)
        squared[:, c * width : (c + 1) * width] = (up * up).astype(jnp.bfloat16)
    total = scatter(squared[...], down_w, waits_down, sums_b, land_b, send_b, recv_b)
    layer_out[...] = (mine.astype(jnp.float32) + total).astype(jnp.bfloat16)
    for cp in pending:
        cp.wait_send()


def mix_channels(peers, heads_out, tokens, mlp_gain, w_out, w_up, w_down):
    rows, part = tokens.shape
    inner, hid = w_out.shape[0], w_up.shape[1]
    width = min(1024, hid)
    f32, bf16 = jnp.float32, jnp.bfloat16
    vmem = pl.BlockSpec(memory_space=pltpu.VMEM)
    hbm = pl.BlockSpec(memory_space=pl.ANY)
    sems = pltpu.SemaphoreType.DMA((peers,))
    return pl.pallas_call(
        functools.partial(mixer_kernel, peers),
        out_shape=jax.ShapeDtypeStruct((rows, part), bf16),
        in_specs=[vmem] * 3 + [hbm] * 3,
        out_specs=vmem,
        scratch_shapes=[
            pltpu.VMEM((peers, inner, part), bf16),
            pltpu.VMEM((peers, hid // width, part, width), bf16),
            pltpu.VMEM((peers, hid, part), bf16),
            pltpu.VMEM((peers, rows, part), f32),
            pltpu.VMEM((peers, rows, part), f32),
            pltpu.VMEM((rows, part), bf16),
            pltpu.VMEM((peers, rows, part), bf16),
            pltpu.VMEM((hid // width, rows, width), f32),
            pltpu.VMEM((rows, hid), bf16),
            pltpu.VMEM((peers, rows, part), f32),
            pltpu.VMEM((peers, rows, part), f32),
            sems,
            pltpu.SemaphoreType.DMA((peers, hid // width)),
            sems,
            sems,
            sems,
            sems,
            sems,
            sems,
            sems,
        ],
        compiler_params=pltpu.CompilerParams(
            collective_id=1, has_side_effects=True, vmem_limit_bytes=VMEM_LIMIT
        ),
        name="mix_channels",
    )(heads_out, tokens, mlp_gain[None, :], w_out, w_up, w_down)


def local_kernels(
    peers,
    tokens,
    mix_gain,
    w_gate,
    w_value,
    w_maps,
    w_step,
    conv_value,
    conv_maps,
    past_value,
    past_maps,
    step_bias,
    decay_log,
    skip_gain,
    head_gain,
    state,
    w_out,
    mlp_gain,
    w_up,
    w_down,
):
    gate, value_new, maps_new, step, decay = project(
        peers, tokens, mix_gain, w_step, step_bias, decay_log, w_gate, w_value, w_maps
    )
    heads_out, state_next, value_tail, maps_tail = step_state(
        decay,
        skip_gain,
        state,
        gate,
        value_new,
        maps_new,
        step,
        past_value,
        past_maps,
        conv_value,
        conv_maps,
        head_gain,
    )
    layer_out = mix_channels(peers, heads_out, tokens, mlp_gain, w_out, w_up, w_down)
    return layer_out, state_next, value_tail, maps_tail


def kernels_fit(peers, tokens, state, w_maps, w_up):
    rows, part = tokens.shape
    heads = state.shape[1]
    inner = heads * HEAD_DIM
    width = min(1024, inner)
    held = 2 * tokens.shape[1] * peers * (2 * inner + w_maps.shape[1])
    return (
        peers > 1
        and rows % 8 == 0
        and part % 128 == 0
        and heads % 2 == 0
        and w_maps.shape[1] == heads * 2 * STATE
        and inner % width == 0
        and width % 128 == 0
        and w_up.shape[1] % min(1024, w_up.shape[1]) == 0
        and w_up.shape[1] % 128 == 0
        and held <= 32 * 1024 * 1024
    )


def rms_rows(matrix, gain_vec):
    widened = matrix.astype(jnp.float32)
    inv_scale = lax.rsqrt(jnp.mean(widened * widened, axis=-1, keepdims=True) + NORM_EPS)
    return (widened * inv_scale * gain_vec).astype(jnp.bfloat16)


def short_conv(past_rows, newest, kernel):
    window = jnp.concatenate([past_rows, newest[:, None, :]], axis=1)
    summed = jnp.sum(window.astype(jnp.float32) * kernel[None], axis=1)
    return (jax.nn.silu(summed), window[:, 1:, :])


def local(
    tokens,
    mix_gain,
    w_gate,
    w_value,
    w_maps,
    w_step,
    conv_value,
    conv_maps,
    past_value,
    past_maps,
    step_bias,
    decay_log,
    skip_gain,
    head_gain,
    state,
    w_out,
    mlp_gain,
    w_up,
    w_down,
):
    whole_rows = lax.all_gather(tokens, "kv", axis=1, tiled=True)
    batch_rows = whole_rows.shape[0]
    heads_here = state.shape[1]
    head_start = lax.axis_index("kv") * heads_here
    normed = rms_rows(whole_rows, mix_gain)
    gate_pre = jnp.dot(normed, w_gate, preferred_element_type=jnp.float32)
    step_cols = lax.dynamic_slice_in_dim(w_step, head_start, heads_here, 1)
    step_pre = jnp.dot(normed, step_cols, preferred_element_type=jnp.float32)
    value_new = jnp.dot(normed, w_value, preferred_element_type=jnp.float32).astype(jnp.bfloat16)
    maps_new = jnp.dot(normed, w_maps, preferred_element_type=jnp.float32).astype(jnp.bfloat16)
    value_act, value_tail = short_conv(past_value, value_new, conv_value)
    maps_act, maps_tail = short_conv(past_maps, maps_new, conv_maps)
    maps_act = lax.optimization_barrier(maps_act.astype(jnp.bfloat16))
    grouped = maps_act.astype(jnp.float32).reshape(batch_rows, -1, 2, STATE)
    per_group = heads_here // grouped.shape[1]
    in_map = jnp.repeat(grouped[:, :, 0], per_group, axis=1)
    out_map = jnp.repeat(grouped[:, :, 1], per_group, axis=1)
    head_values = value_act.reshape(batch_rows, heads_here, HEAD_DIM)
    step_size = jax.nn.softplus(step_pre + step_bias)
    decay_rate = jnp.exp(-step_size * jnp.exp(decay_log))
    written = (step_size[:, :, None] * head_values)[:, :, :, None] * in_map[:, :, None, :]
    state_next = decay_rate[:, :, None, None] * state + written
    read_out = (
        jnp.sum(state_next * out_map[:, :, None, :], axis=-1)
        + skip_gain[None, :, None] * head_values
    )
    gated_heads = read_out * jax.nn.silu(gate_pre.reshape(batch_rows, heads_here, HEAD_DIM))
    inv_scale = lax.rsqrt(jnp.mean(gated_heads * gated_heads, axis=-1, keepdims=True) + NORM_EPS)
    heads_out = gated_heads * inv_scale * head_gain.reshape(heads_here, HEAD_DIM)
    heads_out = heads_out.reshape(batch_rows, heads_here * HEAD_DIM).astype(jnp.bfloat16)
    partial_value = jnp.dot(heads_out, w_out, preferred_element_type=jnp.float32)
    own_part = lax.psum_scatter(partial_value, "kv", scatter_dimension=1, tiled=True)
    own_hidden = lax.optimization_barrier(
        (tokens.astype(jnp.float32) + own_part).astype(jnp.bfloat16)
    )
    hidden = lax.all_gather(own_hidden, "kv", axis=1, tiled=True)
    normed_mlp = rms_rows(hidden, mlp_gain)
    squared = jnp.square(jax.nn.relu(jnp.dot(normed_mlp, w_up, preferred_element_type=jnp.float32)))
    squared = squared.astype(jnp.bfloat16)
    partial_mlp = jnp.dot(squared, w_down, preferred_element_type=jnp.float32)
    mlp_part = lax.psum_scatter(partial_mlp, "kv", scatter_dimension=1, tiled=True)
    layer_out = (own_hidden.astype(jnp.float32) + mlp_part).astype(jnp.bfloat16)
    return (layer_out, state_next, value_tail, maps_tail)


def solution(mesh):
    in_specs = (
        P(("dp", "tp"), "kv"),
        P(),
        P(None, "kv"),
        P(None, "kv"),
        P(None, "kv"),
        P(),
        P(None, "kv"),
        P(None, "kv"),
        P(("dp", "tp"), None, "kv"),
        P(("dp", "tp"), None, "kv"),
        P("kv"),
        P("kv"),
        P("kv"),
        P("kv"),
        P(("dp", "tp"), "kv", None, None),
        P("kv", None),
        P(),
        P(None, "kv"),
        P("kv", None),
    )
    out_specs = (
        P(("dp", "tp"), "kv"),
        P(("dp", "tp"), "kv", None, None),
        P(("dp", "tp"), None, "kv"),
        P(("dp", "tp"), None, "kv"),
    )
    peers = mesh.shape["kv"]

    def device_part(*args):
        if kernels_fit(peers, args[0], args[14], args[4], args[17]):
            return local_kernels(peers, *args)
        return local(*args)

    return jax.shard_map(
        device_part, mesh=mesh, in_specs=in_specs, out_specs=out_specs, check_vma=False
    )
```

```python
import functools

import jax
import jax.numpy as jnp
from jax import lax
from jax.experimental import pallas as pl
from jax.experimental.pallas import tpu as pltpu
from jax.sharding import PartitionSpec as P

HEAD_DIM = 64
STATE = 128
MESH = pl.DeviceIdType.MESH
VMEM_LIMIT = 60 * 1024 * 1024


NORM_EPS = 1e-05
NT = (((1,), (1,)), ((), ()))


def greet(peers, me):
    for d in range(1, peers):
        pl.semaphore_signal(
            pltpu.get_barrier_semaphore(),
            inc=1,
            device_id={"kv": lax.rem(me + d, peers)},
            device_id_type=MESH,
        )


def all_here(peers):
    pl.semaphore_wait(pltpu.get_barrier_semaphore(), peers - 1)


def far_first(peers):
    return sorted(range(1, peers), key=lambda d: -min(d, peers - d))


def push(src, dst, send_sem, recv_sem, target):
    return pltpu.make_async_remote_copy(
        src_ref=src,
        dst_ref=dst,
        send_sem=send_sem,
        recv_sem=recv_sem,
        device_id={"kv": target},
        device_id_type=MESH,
    )


def project_kernel(
    peers,
    tokens,
    gain,
    w_step,
    bias,
    decay_log,
    w_gate,
    w_value,
    normed_out,
    gate_out,
    value_out,
    step_out,
    decay_out,
    slots,
    weights,
    w_sem,
    send_sem,
    recv_sem,
):
    me = lax.axis_index("kv")
    rows, part = tokens.shape
    chunks, width = weights.shape[0], weights.shape[2]
    heads = decay_out.shape[1]
    half = chunks // 2

    greet(peers, me)
    loads = []
    for c in range(chunks):
        ref = w_gate if c < half else w_value
        cp = pltpu.make_async_copy(
            ref.at[:, pl.ds((c % half) * width, width)], weights.at[c], w_sem.at[c]
        )
        cp.start()
        loads.append(cp)

    all_here(peers)
    sends = []
    for d in far_first(peers):
        cp = push(
            tokens,
            slots.at[peers - d],
            send_sem.at[d],
            recv_sem.at[peers - d],
            lax.rem(me + d, peers),
        )
        cp.start()
        sends.append(cp)

    def place(d):
        return pl.multiple_of(lax.rem(me + d, peers) * part, part)

    squares = jnp.zeros((rows, 1), jnp.float32)
    raws = []
    for d in [0] + far_first(peers)[::-1]:
        if d > 0:
            push(tokens, slots.at[d], send_sem.at[d], recv_sem.at[d], me).wait_recv()
        raw = (tokens[...] if d == 0 else slots[d]).astype(jnp.float32)
        squares = squares + jnp.sum(raw * raw, axis=1, keepdims=True)
        raws.append((d, raw))
    inv = lax.rsqrt(squares / (peers * part) + NORM_EPS)
    for d, raw in raws:
        normed_out[:, pl.ds(place(d), part)] = (
            raw * inv * gain[:, pl.ds(place(d), part)]
        ).astype(jnp.bfloat16)

    normed = normed_out[...]
    step_pre = lax.dot_general(normed, w_step[...], NT, preferred_element_type=jnp.float32)
    for c in range(chunks):
        loads[c].wait()
        out = jnp.dot(normed, weights[c], preferred_element_type=jnp.float32)
        at = pl.ds((c % half) * width, width)
        if c < half:
            gate_out[:, at] = out
        else:
            value_out[:, at] = out.astype(jnp.bfloat16)
    own = step_pre[:, :heads]
    for j in range(1, peers):
        own = jnp.where(me == j, step_pre[:, j * heads : (j + 1) * heads], own)
    own = own + bias[...]
    step = jnp.maximum(own, 0.0) + jnp.log1p(jnp.exp(-jnp.abs(own)))
    decay_out[...] = jnp.exp(-step * jnp.exp(decay_log[...]))
    lane = lax.broadcasted_iota(jnp.int32, (rows, 2 * HEAD_DIM), 1)
    for h in range(0, heads, 2):
        step_out[:, h * HEAD_DIM : (h + 2) * HEAD_DIM] = jnp.where(
            lane < HEAD_DIM, step[:, h : h + 1], step[:, h + 1 : h + 2]
        )
    for cp in sends:
        cp.wait_send()


def project(peers, tokens, mix_gain, w_step, step_bias, decay_log, w_gate, w_value):
    rows, part = tokens.shape
    heads = step_bias.shape[0]
    model, inner = w_value.shape
    width = min(512, inner)
    chunks = 2 * inner // width
    f32, bf16 = jnp.float32, jnp.bfloat16
    vmem = pl.BlockSpec(memory_space=pltpu.VMEM)
    hbm = pl.BlockSpec(memory_space=pl.ANY)
    return pl.pallas_call(
        functools.partial(project_kernel, peers),
        out_shape=(
            jax.ShapeDtypeStruct((rows, model), bf16),
            jax.ShapeDtypeStruct((rows, inner), f32),
            jax.ShapeDtypeStruct((rows, inner), bf16),
            jax.ShapeDtypeStruct((rows, inner), f32),
            jax.ShapeDtypeStruct((rows, heads), f32),
        ),
        in_specs=[vmem] * 5 + [hbm] * 2,
        out_specs=(vmem,) * 5,
        scratch_shapes=[
            pltpu.VMEM((peers, rows, part), bf16),
            pltpu.VMEM((chunks, model, width), bf16),
            pltpu.SemaphoreType.DMA((chunks,)),
            pltpu.SemaphoreType.DMA((peers,)),
            pltpu.SemaphoreType.DMA((peers,)),
        ],
        compiler_params=pltpu.CompilerParams(
            collective_id=0, has_side_effects=True, vmem_limit_bytes=VMEM_LIMIT
        ),
        name="project",
    )(
        tokens,
        mix_gain[None, :],
        w_step.T,
        step_bias[None, :],
        decay_log[None, :],
        w_gate,
        w_value,
    )


def silu(x):
    return x * jax.nn.sigmoid(x)


def state_kernel(
    decay,
    skip,
    state,
    gate,
    value_new,
    normed,
    w_maps,
    step,
    past_value,
    past_maps,
    conv_value,
    conv_maps,
    head_gain,
    heads_out,
    state_out,
    value_tail,
    maps_tail,
):
    i = pl.program_id(0)
    rows = state.shape[0]

    def conv(past, new, taps, tail):
        taps_n = past.shape[0]
        total = new.astype(jnp.float32) * taps[taps_n : taps_n + 1, :]
        for k in range(taps_n):
            row = past[k]
            total = total + row.astype(jnp.float32) * taps[k : k + 1, :]
            if k > 0:
                tail[k - 1] = row
        tail[taps_n - 1] = new
        return silu(total)

    maps_new = jnp.dot(normed[...], w_maps[...], preferred_element_type=jnp.float32)
    maps_new = maps_new.astype(jnp.bfloat16)
    value_act = conv(past_value, value_new[...], conv_value, value_tail)
    maps_act = conv(past_maps, maps_new, conv_maps, maps_tail)
    maps_act = maps_act.astype(jnp.bfloat16).astype(jnp.float32)

    scaled = value_act * step[...]
    high = scaled.astype(jnp.bfloat16).astype(jnp.float32)
    both = jnp.concatenate([high, scaled - high], axis=0).T.astype(jnp.bfloat16)
    ins = []
    outs = []
    for hh in range(2):
        at = 2 * hh * STATE
        ins.append(jnp.concatenate([maps_act[:, at : at + STATE]] * 2, axis=0))
        outs.append(maps_act[:, at + STATE : at + 2 * STATE])
    readers = jnp.concatenate(outs, axis=0).astype(jnp.bfloat16)

    row = lax.broadcasted_iota(jnp.int32, (2 * rows, STATE), 0)
    lane = lax.broadcasted_iota(jnp.int32, (2 * rows, STATE), 1)
    seq = jnp.where(row >= rows, row - rows, row)
    owner = jnp.where((row >= rows) == (lane >= HEAD_DIM), seq, -1)
    read = jnp.zeros((2 * rows, 2 * HEAD_DIM), jnp.float32)
    for b in range(0, rows, 2):
        fresh = [None] * 4
        for hh in range(2):
            spread = jnp.concatenate(
                [jnp.where(seq == b + k, ins[hh], 0.0) for k in range(2)], axis=1
            ).astype(jnp.bfloat16)
            written = jnp.dot(
                both[hh * HEAD_DIM : (hh + 1) * HEAD_DIM],
                spread,
                preferred_element_type=jnp.float32,
            )
            for k in range(2):
                new = (
                    decay[b + k, 2 * i + hh] * state[b + k, hh]
                    + written[:, k * STATE : (k + 1) * STATE]
                )
                state_out[b + k, hh] = new
                fresh[2 * k + hh] = new.astype(jnp.bfloat16)
        found = lax.dot_general(
            readers, jnp.concatenate(fresh, axis=0), NT, preferred_element_type=jnp.float32
        )
        for k in range(2):
            read = read + jnp.where(
                owner == b + k, found[:, k * 2 * HEAD_DIM : (k + 1) * 2 * HEAD_DIM], 0.0
            )
    first = lane[:rows] < HEAD_DIM
    read_out = read[:rows] + read[rows:]
    read_out = read_out + jnp.where(first, skip[2 * i], skip[2 * i + 1]) * value_act
    gated = read_out * silu(gate[...])
    square = gated * gated
    low = jnp.sum(jnp.where(first, square, 0.0), axis=1, keepdims=True)
    top = jnp.sum(jnp.where(first, 0.0, square), axis=1, keepdims=True)
    inv = lax.rsqrt(jnp.where(first, low, top) / HEAD_DIM + NORM_EPS)
    heads_out[...] = (gated * inv * head_gain[...]).astype(jnp.bfloat16)


def step_state(
    decay,
    skip_gain,
    state,
    gate,
    value_new,
    normed,
    w_maps,
    step,
    past_value,
    past_maps,
    conv_value,
    conv_maps,
    head_gain,
):
    rows, heads = state.shape[:2]
    smem = pl.BlockSpec(memory_space=pltpu.SMEM)
    pair = 2 * HEAD_DIM
    wide = 4 * STATE
    taps = conv_value.shape[0]
    past_v = jnp.swapaxes(past_value, 0, 1)
    past_m = jnp.swapaxes(past_maps, 0, 1)
    flat = lambda width: pl.BlockSpec((rows, width), lambda i: (0, i))
    conv_spec = lambda width: pl.BlockSpec((taps, width), lambda i: (0, i))
    past_spec = lambda width: pl.BlockSpec((taps - 1, rows, width), lambda i: (0, 0, i))
    state_spec = pl.BlockSpec((rows, 2, HEAD_DIM, STATE), lambda i: (0, i, 0, 0))
    heads_out, state_next, tail_v, tail_m = pl.pallas_call(
        state_kernel,
        grid=(heads // 2,),
        out_shape=(
            jax.ShapeDtypeStruct((rows, heads * HEAD_DIM), jnp.bfloat16),
            jax.ShapeDtypeStruct(state.shape, jnp.float32),
            jax.ShapeDtypeStruct(past_v.shape, jnp.bfloat16),
            jax.ShapeDtypeStruct(past_m.shape, jnp.bfloat16),
        ),
        in_specs=[
            smem,
            smem,
            state_spec,
            flat(pair),
            flat(pair),
            pl.BlockSpec(normed.shape, lambda i: (0, 0)),
            pl.BlockSpec((w_maps.shape[0], wide), lambda i: (0, i)),
            flat(pair),
            past_spec(pair),
            past_spec(wide),
            conv_spec(pair),
            conv_spec(wide),
            pl.BlockSpec((1, pair), lambda i: (0, i)),
        ],
        out_specs=(flat(pair), state_spec, past_spec(pair), past_spec(wide)),
        compiler_params=pltpu.CompilerParams(
            dimension_semantics=("arbitrary",), vmem_limit_bytes=VMEM_LIMIT
        ),
        name="step_state",
    )(
        decay,
        skip_gain,
        state,
        gate,
        value_new,
        normed,
        w_maps,
        step,
        past_v,
        past_m,
        conv_value,
        conv_maps,
        head_gain[None, :],
    )
    return heads_out, state_next, jnp.swapaxes(tail_v, 0, 1), jnp.swapaxes(tail_m, 0, 1)


def mixer_kernel(
    peers,
    heads,
    tokens,
    gain,
    w_out,
    w_up,
    w_down,
    layer_out,
    out_w,
    up_w,
    down_w,
    sums_a,
    land_a,
    own_hidden,
    hidden,
    up_acc,
    squared,
    sums_b,
    land_b,
    out_sem,
    up_sem,
    down_sem,
    send_a,
    recv_a,
    send_h,
    recv_h,
    send_b,
    recv_b,
):
    me = lax.axis_index("kv")
    rows, part = tokens.shape
    n_up, width = up_w.shape[1], up_w.shape[3]

    def place(d):
        return pl.multiple_of(lax.rem(me + d, peers) * part, part)

    order = far_first(peers) + [0]
    greet(peers, me)
    waits_out, waits_down = {}, {}
    for d in order:
        cp = pltpu.make_async_copy(w_out.at[:, pl.ds(place(d), part)], out_w.at[d], out_sem.at[d])
        cp.start()
        waits_out[d] = cp
    for d in range(peers):
        for c in range(n_up):
            pltpu.make_async_copy(
                w_up.at[pl.ds(place(d), part), pl.ds(c * width, width)],
                up_w.at[d, c],
                up_sem.at[d, c],
            ).start()
    for d in order:
        cp = pltpu.make_async_copy(
            w_down.at[:, pl.ds(place(d), part)], down_w.at[d], down_sem.at[d]
        )
        cp.start()
        waits_down[d] = cp

    pending = []

    def scatter(left, weights, waits, sums, land, send, recv):
        for d in order:
            waits[d].wait()
            piece = jnp.dot(left, weights[d], preferred_element_type=jnp.float32)
            if d == 0:
                total = piece
            else:
                sums[d] = piece.astype(jnp.bfloat16)
                if not pending:
                    all_here(peers)
                cp = push(
                    sums.at[d],
                    land.at[peers - d],
                    send.at[d],
                    recv.at[peers - d],
                    lax.rem(me + d, peers),
                )
                cp.start()
                pending.append(cp)
        for d in range(1, peers):
            push(sums.at[d], land.at[d], send.at[d], recv.at[d], me).wait_recv()
            total = total + land[d].astype(jnp.float32)
        return total

    total = scatter(heads[...], out_w, waits_out, sums_a, land_a, send_a, recv_a)
    mine = (tokens[...].astype(jnp.float32) + total).astype(jnp.bfloat16)
    own_hidden[...] = mine
    for d in range(1, peers):
        cp = push(
            own_hidden,
            hidden.at[peers - d],
            send_h.at[d],
            recv_h.at[peers - d],
            lax.rem(me + d, peers),
        )
        cp.start()
        pending.append(cp)

    squares = jnp.zeros((rows, 1), jnp.float32)
    for d in range(peers):
        if d == 0:
            raw = mine
        else:
            push(own_hidden, hidden.at[d], send_h.at[d], recv_h.at[d], me).wait_recv()
            raw = hidden[d]
        wide = raw.astype(jnp.float32)
        squares = squares + jnp.sum(wide * wide, axis=1, keepdims=True)
        scaled = wide * gain[:, pl.ds(place(d), part)]
        high = scaled.astype(jnp.bfloat16).astype(jnp.float32)
        scaled = jnp.concatenate([high, scaled - high], axis=0).astype(jnp.bfloat16)

        def chunk(c, carry, d=d, scaled=scaled):
            pltpu.make_async_copy(
                w_up.at[pl.ds(0, part), pl.ds(0, width)], up_w.at[d, c], up_sem.at[d, c]
            ).wait()
            out = jnp.dot(scaled, up_w[d, c], preferred_element_type=jnp.float32)
            out = out[:rows] + out[rows:]
            up_acc[c] = out if d == 0 else up_acc[c] + out
            return carry

        lax.fori_loop(0, n_up, chunk, 0)

    inv = lax.rsqrt(squares / (peers * part) + NORM_EPS)
    for c in range(n_up):
        up = jnp.maximum(up_acc[c] * inv, 0.0)
        squared[:, c * width : (c + 1) * width] = (up * up).astype(jnp.bfloat16)
    total = scatter(squared[...], down_w, waits_down, sums_b, land_b, send_b, recv_b)
    layer_out[...] = (mine.astype(jnp.float32) + total).astype(jnp.bfloat16)
    for cp in pending:
        cp.wait_send()


def mix_channels(peers, heads_out, tokens, mlp_gain, w_out, w_up, w_down):
    rows, part = tokens.shape
    inner, hid = w_out.shape[0], w_up.shape[1]
    width = min(2048, hid)
    f32, bf16 = jnp.float32, jnp.bfloat16
    vmem = pl.BlockSpec(memory_space=pltpu.VMEM)
    hbm = pl.BlockSpec(memory_space=pl.ANY)
    sems = pltpu.SemaphoreType.DMA((peers,))
    return pl.pallas_call(
        functools.partial(mixer_kernel, peers),
        out_shape=jax.ShapeDtypeStruct((rows, part), bf16),
        in_specs=[vmem] * 3 + [hbm] * 3,
        out_specs=vmem,
        scratch_shapes=[
            pltpu.VMEM((peers, inner, part), bf16),
            pltpu.VMEM((peers, hid // width, part, width), bf16),
            pltpu.VMEM((peers, hid, part), bf16),
            pltpu.VMEM((peers, rows, part), bf16),
            pltpu.VMEM((peers, rows, part), bf16),
            pltpu.VMEM((rows, part), bf16),
            pltpu.VMEM((peers, rows, part), bf16),
            pltpu.VMEM((hid // width, rows, width), f32),
            pltpu.VMEM((rows, hid), bf16),
            pltpu.VMEM((peers, rows, part), bf16),
            pltpu.VMEM((peers, rows, part), bf16),
            sems,
            pltpu.SemaphoreType.DMA((peers, hid // width)),
            sems,
            sems,
            sems,
            sems,
            sems,
            sems,
            sems,
        ],
        compiler_params=pltpu.CompilerParams(
            collective_id=1, has_side_effects=True, vmem_limit_bytes=VMEM_LIMIT
        ),
        name="mix_channels",
    )(heads_out, tokens, mlp_gain[None, :], w_out, w_up, w_down)


def local_kernels(
    peers,
    tokens,
    mix_gain,
    w_gate,
    w_value,
    w_maps,
    w_step,
    conv_value,
    conv_maps,
    past_value,
    past_maps,
    step_bias,
    decay_log,
    skip_gain,
    head_gain,
    state,
    w_out,
    mlp_gain,
    w_up,
    w_down,
):
    normed, gate, value_new, step, decay = project(
        peers, tokens, mix_gain, w_step, step_bias, decay_log, w_gate, w_value
    )
    heads_out, state_next, value_tail, maps_tail = step_state(
        decay,
        skip_gain,
        state,
        gate,
        value_new,
        normed,
        w_maps,
        step,
        past_value,
        past_maps,
        conv_value,
        conv_maps,
        head_gain,
    )
    layer_out = mix_channels(peers, heads_out, tokens, mlp_gain, w_out, w_up, w_down)
    return layer_out, state_next, value_tail, maps_tail


def kernels_fit(peers, tokens, state, w_maps, w_up):
    rows, part = tokens.shape
    heads = state.shape[1]
    inner = heads * HEAD_DIM
    width = min(512, inner)
    held = 2 * tokens.shape[1] * peers * (2 * inner + w_maps.shape[1])
    return (
        peers > 1
        and rows % 8 == 0
        and part % 128 == 0
        and heads % 2 == 0
        and w_maps.shape[1] == heads * 2 * STATE
        and inner % width == 0
        and width % 128 == 0
        and w_up.shape[1] % min(2048, w_up.shape[1]) == 0
        and w_up.shape[1] % 128 == 0
        and held <= 32 * 1024 * 1024
    )


def rms_rows(matrix, gain_vec):
    widened = matrix.astype(jnp.float32)
    inv_scale = lax.rsqrt(jnp.mean(widened * widened, axis=-1, keepdims=True) + NORM_EPS)
    return (widened * inv_scale * gain_vec).astype(jnp.bfloat16)


def short_conv(past_rows, newest, kernel):
    window = jnp.concatenate([past_rows, newest[:, None, :]], axis=1)
    summed = jnp.sum(window.astype(jnp.float32) * kernel[None], axis=1)
    return (jax.nn.silu(summed), window[:, 1:, :])


def local(
    tokens,
    mix_gain,
    w_gate,
    w_value,
    w_maps,
    w_step,
    conv_value,
    conv_maps,
    past_value,
    past_maps,
    step_bias,
    decay_log,
    skip_gain,
    head_gain,
    state,
    w_out,
    mlp_gain,
    w_up,
    w_down,
):
    whole_rows = lax.all_gather(tokens, "kv", axis=1, tiled=True)
    batch_rows = whole_rows.shape[0]
    heads_here = state.shape[1]
    head_start = lax.axis_index("kv") * heads_here
    normed = rms_rows(whole_rows, mix_gain)
    gate_pre = jnp.dot(normed, w_gate, preferred_element_type=jnp.float32)
    step_cols = lax.dynamic_slice_in_dim(w_step, head_start, heads_here, 1)
    step_pre = jnp.dot(normed, step_cols, preferred_element_type=jnp.float32)
    value_new = jnp.dot(normed, w_value, preferred_element_type=jnp.float32).astype(jnp.bfloat16)
    maps_new = jnp.dot(normed, w_maps, preferred_element_type=jnp.float32).astype(jnp.bfloat16)
    value_act, value_tail = short_conv(past_value, value_new, conv_value)
    maps_act, maps_tail = short_conv(past_maps, maps_new, conv_maps)
    maps_act = lax.optimization_barrier(maps_act.astype(jnp.bfloat16))
    grouped = maps_act.astype(jnp.float32).reshape(batch_rows, -1, 2, STATE)
    per_group = heads_here // grouped.shape[1]
    in_map = jnp.repeat(grouped[:, :, 0], per_group, axis=1)
    out_map = jnp.repeat(grouped[:, :, 1], per_group, axis=1)
    head_values = value_act.reshape(batch_rows, heads_here, HEAD_DIM)
    step_size = jax.nn.softplus(step_pre + step_bias)
    decay_rate = jnp.exp(-step_size * jnp.exp(decay_log))
    written = (step_size[:, :, None] * head_values)[:, :, :, None] * in_map[:, :, None, :]
    state_next = decay_rate[:, :, None, None] * state + written
    read_out = (
        jnp.sum(state_next * out_map[:, :, None, :], axis=-1)
        + skip_gain[None, :, None] * head_values
    )
    gated_heads = read_out * jax.nn.silu(gate_pre.reshape(batch_rows, heads_here, HEAD_DIM))
    inv_scale = lax.rsqrt(jnp.mean(gated_heads * gated_heads, axis=-1, keepdims=True) + NORM_EPS)
    heads_out = gated_heads * inv_scale * head_gain.reshape(heads_here, HEAD_DIM)
    heads_out = heads_out.reshape(batch_rows, heads_here * HEAD_DIM).astype(jnp.bfloat16)
    partial_value = jnp.dot(heads_out, w_out, preferred_element_type=jnp.float32)
    own_part = lax.psum_scatter(partial_value, "kv", scatter_dimension=1, tiled=True)
    own_hidden = lax.optimization_barrier(
        (tokens.astype(jnp.float32) + own_part).astype(jnp.bfloat16)
    )
    hidden = lax.all_gather(own_hidden, "kv", axis=1, tiled=True)
    normed_mlp = rms_rows(hidden, mlp_gain)
    squared = jnp.square(jax.nn.relu(jnp.dot(normed_mlp, w_up, preferred_element_type=jnp.float32)))
    squared = squared.astype(jnp.bfloat16)
    partial_mlp = jnp.dot(squared, w_down, preferred_element_type=jnp.float32)
    mlp_part = lax.psum_scatter(partial_mlp, "kv", scatter_dimension=1, tiled=True)
    layer_out = (own_hidden.astype(jnp.float32) + mlp_part).astype(jnp.bfloat16)
    return (layer_out, state_next, value_tail, maps_tail)


def solution(mesh):
    in_specs = (
        P(("dp", "tp"), "kv"),
        P(),
        P(None, "kv"),
        P(None, "kv"),
        P(None, "kv"),
        P(),
        P(None, "kv"),
        P(None, "kv"),
        P(("dp", "tp"), None, "kv"),
        P(("dp", "tp"), None, "kv"),
        P("kv"),
        P("kv"),
        P("kv"),
        P("kv"),
        P(("dp", "tp"), "kv", None, None),
        P("kv", None),
        P(),
        P(None, "kv"),
        P("kv", None),
    )
    out_specs = (
        P(("dp", "tp"), "kv"),
        P(("dp", "tp"), "kv", None, None),
        P(("dp", "tp"), None, "kv"),
        P(("dp", "tp"), None, "kv"),
    )
    peers = mesh.shape["kv"]

    def device_part(*args):
        if kernels_fit(peers, args[0], args[14], args[4], args[17]):
            return local_kernels(peers, *args)
        return local(*args)

    return jax.shard_map(
        device_part, mesh=mesh, in_specs=in_specs, out_specs=out_specs, check_vma=False
    )
```

```python
import functools

import jax
import jax.numpy as jnp
from jax import lax
from jax.experimental import pallas as pl
from jax.experimental.pallas import tpu as pltpu
from jax.sharding import PartitionSpec as P

HEAD_DIM = 64
STATE = 128
MESH = pl.DeviceIdType.MESH
VMEM_LIMIT = 60 * 1024 * 1024


NORM_EPS = 1e-05
NT = (((1,), (1,)), ((), ()))


def greet(peers, me):
    for d in range(1, peers):
        pl.semaphore_signal(
            pltpu.get_barrier_semaphore(),
            inc=1,
            device_id={"kv": lax.rem(me + d, peers)},
            device_id_type=MESH,
        )


def all_here(peers):
    pl.semaphore_wait(pltpu.get_barrier_semaphore(), peers - 1)


def far_first(peers):
    return sorted(range(1, peers), key=lambda d: -min(d, peers - d))


def push(src, dst, send_sem, recv_sem, target):
    return pltpu.make_async_remote_copy(
        src_ref=src,
        dst_ref=dst,
        send_sem=send_sem,
        recv_sem=recv_sem,
        device_id={"kv": target},
        device_id_type=MESH,
    )


def project_kernel(
    peers,
    tokens,
    gain,
    w_step,
    bias,
    decay_log,
    w_gate,
    w_value,
    w_maps,
    gate_out,
    value_out,
    maps_out,
    step_out,
    decay_out,
    slots,
    weights,
    acc,
    w_sem,
    send_sem,
    recv_sem,
):
    me = lax.axis_index("kv")
    rows, part = tokens.shape
    chunks, width = weights.shape[1], weights.shape[3]
    heads = decay_out.shape[1]
    inner = value_out.shape[1]
    greet(peers, me)

    for d in [0] + far_first(peers)[::-1]:
        start = pl.multiple_of(lax.rem(me + d, peers) * part, part)
        for k, ref in enumerate((w_gate, w_value)):
            pltpu.make_async_copy(
                ref.at[pl.ds(start, part), :],
                weights.at[d, 0, :, pl.ds(k * inner, inner)],
                w_sem.at[d, 0],
            ).start()
        for c in range(1, chunks):
            pltpu.make_async_copy(
                w_maps.at[pl.ds(start, part), pl.ds((c - 1) * width, width)],
                weights.at[d, c],
                w_sem.at[d, c],
            ).start()

    all_here(peers)
    sends = []
    for d in far_first(peers):
        cp = push(
            tokens,
            slots.at[peers - d],
            send_sem.at[d],
            recv_sem.at[peers - d],
            lax.rem(me + d, peers),
        )
        cp.start()
        sends.append(cp)

    squares = jnp.zeros((rows, 1), jnp.float32)
    step_pre = jnp.zeros((2 * rows, w_step.shape[0]), jnp.float32)
    for d in [0] + far_first(peers)[::-1]:
        start = pl.multiple_of(lax.rem(me + d, peers) * part, part)
        if d == 0:
            raw = tokens[...]
        else:
            push(tokens, slots.at[d], send_sem.at[d], recv_sem.at[d], me).wait_recv()
            raw = slots[d]
        wide = raw.astype(jnp.float32)
        squares = squares + jnp.sum(wide * wide, axis=1, keepdims=True)
        scaled = wide * gain[:, pl.ds(start, part)]
        high = scaled.astype(jnp.bfloat16).astype(jnp.float32)
        scaled = jnp.concatenate([high, scaled - high], axis=0).astype(jnp.bfloat16)
        step_pre = step_pre + lax.dot_general(
            scaled, w_step[:, pl.ds(start, part)], NT, preferred_element_type=jnp.float32
        )

        for c in range(chunks):
            pltpu.make_async_copy(
                w_maps.at[pl.ds(0, part), pl.ds(0, width)], weights.at[d, c], w_sem.at[d, c]
            ).wait()
            out = jnp.dot(scaled, weights[d, c], preferred_element_type=jnp.float32)
            out = out[:rows] + out[rows:]
            acc[c] = out if d == 0 else acc[c] + out

    inv = lax.rsqrt(squares / (peers * part) + NORM_EPS)
    for c in range(chunks):
        total = acc[c] * inv
        if c == 0:
            gate_out[...] = total[:, :inner]
            value_out[...] = total[:, inner:].astype(jnp.bfloat16)
        else:
            maps_out[:, (c - 1) * width : c * width] = total.astype(jnp.bfloat16)
    step_pre = (step_pre[:rows] + step_pre[rows:]) * inv
    own = step_pre[:, :heads]
    for j in range(1, peers):
        own = jnp.where(me == j, step_pre[:, j * heads : (j + 1) * heads], own)
    own = own + bias[...]
    step = jnp.maximum(own, 0.0) + jnp.log1p(jnp.exp(-jnp.abs(own)))
    decay_out[...] = jnp.exp(-step * jnp.exp(decay_log[...]))
    lane = lax.broadcasted_iota(jnp.int32, (rows, 2 * HEAD_DIM), 1)
    for h in range(0, heads, 2):
        step_out[:, h * HEAD_DIM : (h + 2) * HEAD_DIM] = jnp.where(
            lane < HEAD_DIM, step[:, h : h + 1], step[:, h + 1 : h + 2]
        )
    for cp in sends:
        cp.wait_send()


def project(peers, tokens, mix_gain, w_step, step_bias, decay_log, w_gate, w_value, w_maps):
    rows, part = tokens.shape
    heads = step_bias.shape[0]
    inner, maps = w_value.shape[1], w_maps.shape[1]
    width = 2 * inner
    chunks = 1 + maps // width
    f32 = jnp.float32
    vmem = pl.BlockSpec(memory_space=pltpu.VMEM)
    hbm = pl.BlockSpec(memory_space=pl.ANY)
    return pl.pallas_call(
        functools.partial(project_kernel, peers),
        out_shape=(
            jax.ShapeDtypeStruct((rows, inner), f32),
            jax.ShapeDtypeStruct((rows, inner), jnp.bfloat16),
            jax.ShapeDtypeStruct((rows, maps), jnp.bfloat16),
            jax.ShapeDtypeStruct((rows, inner), f32),
            jax.ShapeDtypeStruct((rows, heads), f32),
        ),
        in_specs=[vmem] * 5 + [hbm] * 3,
        out_specs=(vmem,) * 5,
        scratch_shapes=[
            pltpu.VMEM((peers, rows, part), jnp.bfloat16),
            pltpu.VMEM((peers, chunks, part, width), jnp.bfloat16),
            pltpu.VMEM((chunks, rows, width), f32),
            pltpu.SemaphoreType.DMA((peers, chunks)),
            pltpu.SemaphoreType.DMA((peers,)),
            pltpu.SemaphoreType.DMA((peers,)),
        ],
        compiler_params=pltpu.CompilerParams(
            collective_id=0, has_side_effects=True, vmem_limit_bytes=VMEM_LIMIT
        ),
        name="project",
    )(
        tokens,
        mix_gain[None, :],
        w_step.T,
        step_bias[None, :],
        decay_log[None, :],
        w_gate,
        w_value,
        w_maps,
    )


def silu(x):
    return x * jax.nn.sigmoid(x)


def state_kernel(
    decay,
    skip,
    state,
    gate,
    value_new,
    maps_new,
    step,
    past_value,
    past_maps,
    conv_value,
    conv_maps,
    head_gain,
    heads_out,
    state_out,
    value_tail,
    maps_tail,
):
    i = pl.program_id(0)
    rows = state.shape[0]

    def conv(past, new, taps, tail):
        taps_n = past.shape[0]
        total = new[...].astype(jnp.float32) * taps[taps_n : taps_n + 1, :]
        for k in range(taps_n):
            row = past[k]
            total = total + row.astype(jnp.float32) * taps[k : k + 1, :]
            if k > 0:
                tail[k - 1] = row
        tail[taps_n - 1] = new[...]
        return silu(total)

    value_act = conv(past_value, value_new, conv_value, value_tail)
    maps_act = conv(past_maps, maps_new, conv_maps, maps_tail)
    maps_act = maps_act.astype(jnp.bfloat16).astype(jnp.float32)

    scaled = value_act * step[...]
    high = scaled.astype(jnp.bfloat16).astype(jnp.float32)
    both = jnp.concatenate([high, scaled - high], axis=0).T.astype(jnp.bfloat16)
    ins = []
    outs = []
    for hh in range(2):
        at = 2 * hh * STATE
        ins.append(jnp.concatenate([maps_act[:, at : at + STATE]] * 2, axis=0))
        outs.append(maps_act[:, at + STATE : at + 2 * STATE])
    readers = jnp.concatenate(outs, axis=0).astype(jnp.bfloat16)

    row = lax.broadcasted_iota(jnp.int32, (2 * rows, STATE), 0)
    lane = lax.broadcasted_iota(jnp.int32, (2 * rows, STATE), 1)
    seq = jnp.where(row >= rows, row - rows, row)
    owner = jnp.where((row >= rows) == (lane >= HEAD_DIM), seq, -1)
    read = jnp.zeros((2 * rows, 2 * HEAD_DIM), jnp.float32)
    for b in range(0, rows, 2):
        fresh = [None] * 4
        for hh in range(2):
            spread = jnp.concatenate(
                [jnp.where(seq == b + k, ins[hh], 0.0) for k in range(2)], axis=1
            ).astype(jnp.bfloat16)
            written = jnp.dot(
                both[hh * HEAD_DIM : (hh + 1) * HEAD_DIM],
                spread,
                preferred_element_type=jnp.float32,
            )
            for k in range(2):
                new = (
                    decay[b + k, 2 * i + hh] * state[b + k, hh]
                    + written[:, k * STATE : (k + 1) * STATE]
                )
                state_out[b + k, hh] = new
                fresh[2 * k + hh] = new.astype(jnp.bfloat16)
        found = lax.dot_general(
            readers, jnp.concatenate(fresh, axis=0), NT, preferred_element_type=jnp.float32
        )
        for k in range(2):
            read = read + jnp.where(
                owner == b + k, found[:, k * 2 * HEAD_DIM : (k + 1) * 2 * HEAD_DIM], 0.0
            )
    first = lane[:rows] < HEAD_DIM
    read_out = read[:rows] + read[rows:]
    read_out = read_out + jnp.where(first, skip[2 * i], skip[2 * i + 1]) * value_act
    gated = read_out * silu(gate[...])
    square = gated * gated
    low = jnp.sum(jnp.where(first, square, 0.0), axis=1, keepdims=True)
    top = jnp.sum(jnp.where(first, 0.0, square), axis=1, keepdims=True)
    inv = lax.rsqrt(jnp.where(first, low, top) / HEAD_DIM + NORM_EPS)
    heads_out[...] = (gated * inv * head_gain[...]).astype(jnp.bfloat16)


def step_state(
    decay,
    skip_gain,
    state,
    gate,
    value_new,
    maps_new,
    step,
    past_value,
    past_maps,
    conv_value,
    conv_maps,
    head_gain,
):
    rows, heads = state.shape[:2]
    smem = pl.BlockSpec(memory_space=pltpu.SMEM)
    pair = 2 * HEAD_DIM
    wide = 4 * STATE
    taps = conv_value.shape[0]
    past_v = jnp.swapaxes(past_value, 0, 1)
    past_m = jnp.swapaxes(past_maps, 0, 1)
    flat = lambda width: pl.BlockSpec((rows, width), lambda i: (0, i))
    conv_spec = lambda width: pl.BlockSpec((taps, width), lambda i: (0, i))
    past_spec = lambda width: pl.BlockSpec((taps - 1, rows, width), lambda i: (0, 0, i))
    state_spec = pl.BlockSpec((rows, 2, HEAD_DIM, STATE), lambda i: (0, i, 0, 0))
    heads_out, state_next, tail_v, tail_m = pl.pallas_call(
        state_kernel,
        grid=(heads // 2,),
        out_shape=(
            jax.ShapeDtypeStruct((rows, heads * HEAD_DIM), jnp.bfloat16),
            jax.ShapeDtypeStruct(state.shape, jnp.float32),
            jax.ShapeDtypeStruct(past_v.shape, jnp.bfloat16),
            jax.ShapeDtypeStruct(past_m.shape, jnp.bfloat16),
        ),
        in_specs=[
            smem,
            smem,
            state_spec,
            flat(pair),
            flat(pair),
            flat(wide),
            flat(pair),
            past_spec(pair),
            past_spec(wide),
            conv_spec(pair),
            conv_spec(wide),
            pl.BlockSpec((1, pair), lambda i: (0, i)),
        ],
        out_specs=(flat(pair), state_spec, past_spec(pair), past_spec(wide)),
        compiler_params=pltpu.CompilerParams(
            dimension_semantics=("arbitrary",), vmem_limit_bytes=VMEM_LIMIT
        ),
        name="step_state",
    )(
        decay,
        skip_gain,
        state,
        gate,
        value_new,
        maps_new,
        step,
        past_v,
        past_m,
        conv_value,
        conv_maps,
        head_gain[None, :],
    )
    return heads_out, state_next, jnp.swapaxes(tail_v, 0, 1), jnp.swapaxes(tail_m, 0, 1)


def mixer_kernel(
    peers,
    heads,
    tokens,
    gain,
    w_out,
    w_up,
    w_down,
    layer_out,
    out_w,
    up_w,
    down_w,
    sums_a,
    land_a,
    own_hidden,
    hidden,
    up_acc,
    squared,
    sums_b,
    land_b,
    out_sem,
    up_sem,
    down_sem,
    send_a,
    recv_a,
    send_h,
    recv_h,
    send_b,
    recv_b,
):
    me = lax.axis_index("kv")
    rows, part = tokens.shape
    n_up, width = up_w.shape[1], up_w.shape[3]

    def place(d):
        return pl.multiple_of(lax.rem(me + d, peers) * part, part)

    order = far_first(peers) + [0]
    greet(peers, me)
    waits_out, waits_down = {}, {}
    for d in order:
        cp = pltpu.make_async_copy(w_out.at[:, pl.ds(place(d), part)], out_w.at[d], out_sem.at[d])
        cp.start()
        waits_out[d] = cp
    for d in range(peers):
        for c in range(n_up):
            pltpu.make_async_copy(
                w_up.at[pl.ds(place(d), part), pl.ds(c * width, width)],
                up_w.at[d, c],
                up_sem.at[d, c],
            ).start()
    for d in order:
        cp = pltpu.make_async_copy(
            w_down.at[:, pl.ds(place(d), part)], down_w.at[d], down_sem.at[d]
        )
        cp.start()
        waits_down[d] = cp

    pending = []

    def scatter(left, weights, waits, sums, land, send, recv):
        for d in order:
            waits[d].wait()
            piece = jnp.dot(left, weights[d], preferred_element_type=jnp.float32)
            if d == 0:
                total = piece
            else:
                sums[d] = piece.astype(jnp.bfloat16)
                if not pending:
                    all_here(peers)
                cp = push(
                    sums.at[d],
                    land.at[peers - d],
                    send.at[d],
                    recv.at[peers - d],
                    lax.rem(me + d, peers),
                )
                cp.start()
                pending.append(cp)
        for d in range(1, peers):
            push(sums.at[d], land.at[d], send.at[d], recv.at[d], me).wait_recv()
            total = total + land[d].astype(jnp.float32)
        return total

    total = scatter(heads[...], out_w, waits_out, sums_a, land_a, send_a, recv_a)
    mine = (tokens[...].astype(jnp.float32) + total).astype(jnp.bfloat16)
    own_hidden[...] = mine
    for d in range(1, peers):
        cp = push(
            own_hidden,
            hidden.at[peers - d],
            send_h.at[d],
            recv_h.at[peers - d],
            lax.rem(me + d, peers),
        )
        cp.start()
        pending.append(cp)

    squares = jnp.zeros((rows, 1), jnp.float32)
    for d in range(peers):
        if d == 0:
            raw = mine
        else:
            push(own_hidden, hidden.at[d], send_h.at[d], recv_h.at[d], me).wait_recv()
            raw = hidden[d]
        wide = raw.astype(jnp.float32)
        squares = squares + jnp.sum(wide * wide, axis=1, keepdims=True)
        scaled = wide * gain[:, pl.ds(place(d), part)]
        high = scaled.astype(jnp.bfloat16).astype(jnp.float32)
        scaled = jnp.concatenate([high, scaled - high], axis=0).astype(jnp.bfloat16)

        def chunk(c, carry, d=d, scaled=scaled):
            pltpu.make_async_copy(
                w_up.at[pl.ds(0, part), pl.ds(0, width)], up_w.at[d, c], up_sem.at[d, c]
            ).wait()
            out = jnp.dot(scaled, up_w[d, c], preferred_element_type=jnp.float32)
            out = out[:rows] + out[rows:]
            up_acc[c] = out if d == 0 else up_acc[c] + out
            return carry

        lax.fori_loop(0, n_up, chunk, 0)

    inv = lax.rsqrt(squares / (peers * part) + NORM_EPS)
    for c in range(n_up):
        up = jnp.maximum(up_acc[c] * inv, 0.0)
        squared[:, c * width : (c + 1) * width] = (up * up).astype(jnp.bfloat16)
    total = scatter(squared[...], down_w, waits_down, sums_b, land_b, send_b, recv_b)
    layer_out[...] = (mine.astype(jnp.float32) + total).astype(jnp.bfloat16)
    for cp in pending:
        cp.wait_send()


def mix_channels(peers, heads_out, tokens, mlp_gain, w_out, w_up, w_down):
    rows, part = tokens.shape
    inner, hid = w_out.shape[0], w_up.shape[1]
    width = min(2048, hid)
    f32, bf16 = jnp.float32, jnp.bfloat16
    vmem = pl.BlockSpec(memory_space=pltpu.VMEM)
    hbm = pl.BlockSpec(memory_space=pl.ANY)
    sems = pltpu.SemaphoreType.DMA((peers,))
    return pl.pallas_call(
        functools.partial(mixer_kernel, peers),
        out_shape=jax.ShapeDtypeStruct((rows, part), bf16),
        in_specs=[vmem] * 3 + [hbm] * 3,
        out_specs=vmem,
        scratch_shapes=[
            pltpu.VMEM((peers, inner, part), bf16),
            pltpu.VMEM((peers, hid // width, part, width), bf16),
            pltpu.VMEM((peers, hid, part), bf16),
            pltpu.VMEM((peers, rows, part), bf16),
            pltpu.VMEM((peers, rows, part), bf16),
            pltpu.VMEM((rows, part), bf16),
            pltpu.VMEM((peers, rows, part), bf16),
            pltpu.VMEM((hid // width, rows, width), f32),
            pltpu.VMEM((rows, hid), bf16),
            pltpu.VMEM((peers, rows, part), bf16),
            pltpu.VMEM((peers, rows, part), bf16),
            sems,
            pltpu.SemaphoreType.DMA((peers, hid // width)),
            sems,
            sems,
            sems,
            sems,
            sems,
            sems,
            sems,
        ],
        compiler_params=pltpu.CompilerParams(
            collective_id=1, has_side_effects=True, vmem_limit_bytes=VMEM_LIMIT
        ),
        name="mix_channels",
    )(heads_out, tokens, mlp_gain[None, :], w_out, w_up, w_down)


def local_kernels(
    peers,
    tokens,
    mix_gain,
    w_gate,
    w_value,
    w_maps,
    w_step,
    conv_value,
    conv_maps,
    past_value,
    past_maps,
    step_bias,
    decay_log,
    skip_gain,
    head_gain,
    state,
    w_out,
    mlp_gain,
    w_up,
    w_down,
):
    gate, value_new, maps_new, step, decay = project(
        peers, tokens, mix_gain, w_step, step_bias, decay_log, w_gate, w_value, w_maps
    )
    heads_out, state_next, value_tail, maps_tail = step_state(
        decay,
        skip_gain,
        state,
        gate,
        value_new,
        maps_new,
        step,
        past_value,
        past_maps,
        conv_value,
        conv_maps,
        head_gain,
    )
    layer_out = mix_channels(peers, heads_out, tokens, mlp_gain, w_out, w_up, w_down)
    return layer_out, state_next, value_tail, maps_tail


def kernels_fit(peers, tokens, state, w_maps, w_up):
    rows, part = tokens.shape
    heads = state.shape[1]
    inner = heads * HEAD_DIM
    width = min(1024, inner)
    held = 2 * tokens.shape[1] * peers * (2 * inner + w_maps.shape[1])
    return (
        peers > 1
        and rows % 8 == 0
        and part % 128 == 0
        and heads % 2 == 0
        and w_maps.shape[1] == heads * 2 * STATE
        and inner % width == 0
        and width % 128 == 0
        and w_up.shape[1] % min(2048, w_up.shape[1]) == 0
        and w_up.shape[1] % 128 == 0
        and held <= 32 * 1024 * 1024
    )


def rms_rows(matrix, gain_vec):
    widened = matrix.astype(jnp.float32)
    inv_scale = lax.rsqrt(jnp.mean(widened * widened, axis=-1, keepdims=True) + NORM_EPS)
    return (widened * inv_scale * gain_vec).astype(jnp.bfloat16)


def short_conv(past_rows, newest, kernel):
    window = jnp.concatenate([past_rows, newest[:, None, :]], axis=1)
    summed = jnp.sum(window.astype(jnp.float32) * kernel[None], axis=1)
    return (jax.nn.silu(summed), window[:, 1:, :])


def local(
    tokens,
    mix_gain,
    w_gate,
    w_value,
    w_maps,
    w_step,
    conv_value,
    conv_maps,
    past_value,
    past_maps,
    step_bias,
    decay_log,
    skip_gain,
    head_gain,
    state,
    w_out,
    mlp_gain,
    w_up,
    w_down,
):
    whole_rows = lax.all_gather(tokens, "kv", axis=1, tiled=True)
    batch_rows = whole_rows.shape[0]
    heads_here = state.shape[1]
    head_start = lax.axis_index("kv") * heads_here
    normed = rms_rows(whole_rows, mix_gain)
    gate_pre = jnp.dot(normed, w_gate, preferred_element_type=jnp.float32)
    step_cols = lax.dynamic_slice_in_dim(w_step, head_start, heads_here, 1)
    step_pre = jnp.dot(normed, step_cols, preferred_element_type=jnp.float32)
    value_new = jnp.dot(normed, w_value, preferred_element_type=jnp.float32).astype(jnp.bfloat16)
    maps_new = jnp.dot(normed, w_maps, preferred_element_type=jnp.float32).astype(jnp.bfloat16)
    value_act, value_tail = short_conv(past_value, value_new, conv_value)
    maps_act, maps_tail = short_conv(past_maps, maps_new, conv_maps)
    maps_act = lax.optimization_barrier(maps_act.astype(jnp.bfloat16))
    grouped = maps_act.astype(jnp.float32).reshape(batch_rows, -1, 2, STATE)
    per_group = heads_here // grouped.shape[1]
    in_map = jnp.repeat(grouped[:, :, 0], per_group, axis=1)
    out_map = jnp.repeat(grouped[:, :, 1], per_group, axis=1)
    head_values = value_act.reshape(batch_rows, heads_here, HEAD_DIM)
    step_size = jax.nn.softplus(step_pre + step_bias)
    decay_rate = jnp.exp(-step_size * jnp.exp(decay_log))
    written = (step_size[:, :, None] * head_values)[:, :, :, None] * in_map[:, :, None, :]
    state_next = decay_rate[:, :, None, None] * state + written
    read_out = (
        jnp.sum(state_next * out_map[:, :, None, :], axis=-1)
        + skip_gain[None, :, None] * head_values
    )
    gated_heads = read_out * jax.nn.silu(gate_pre.reshape(batch_rows, heads_here, HEAD_DIM))
    inv_scale = lax.rsqrt(jnp.mean(gated_heads * gated_heads, axis=-1, keepdims=True) + NORM_EPS)
    heads_out = gated_heads * inv_scale * head_gain.reshape(heads_here, HEAD_DIM)
    heads_out = heads_out.reshape(batch_rows, heads_here * HEAD_DIM).astype(jnp.bfloat16)
    partial_value = jnp.dot(heads_out, w_out, preferred_element_type=jnp.float32)
    own_part = lax.psum_scatter(partial_value, "kv", scatter_dimension=1, tiled=True)
    own_hidden = lax.optimization_barrier(
        (tokens.astype(jnp.float32) + own_part).astype(jnp.bfloat16)
    )
    hidden = lax.all_gather(own_hidden, "kv", axis=1, tiled=True)
    normed_mlp = rms_rows(hidden, mlp_gain)
    squared = jnp.square(jax.nn.relu(jnp.dot(normed_mlp, w_up, preferred_element_type=jnp.float32)))
    squared = squared.astype(jnp.bfloat16)
    partial_mlp = jnp.dot(squared, w_down, preferred_element_type=jnp.float32)
    mlp_part = lax.psum_scatter(partial_mlp, "kv", scatter_dimension=1, tiled=True)
    layer_out = (own_hidden.astype(jnp.float32) + mlp_part).astype(jnp.bfloat16)
    return (layer_out, state_next, value_tail, maps_tail)


def solution(mesh):
    in_specs = (
        P(("dp", "tp"), "kv"),
        P(),
        P(None, "kv"),
        P(None, "kv"),
        P(None, "kv"),
        P(),
        P(None, "kv"),
        P(None, "kv"),
        P(("dp", "tp"), None, "kv"),
        P(("dp", "tp"), None, "kv"),
        P("kv"),
        P("kv"),
        P("kv"),
        P("kv"),
        P(("dp", "tp"), "kv", None, None),
        P("kv", None),
        P(),
        P(None, "kv"),
        P("kv", None),
    )
    out_specs = (
        P(("dp", "tp"), "kv"),
        P(("dp", "tp"), "kv", None, None),
        P(("dp", "tp"), None, "kv"),
        P(("dp", "tp"), None, "kv"),
    )
    peers = mesh.shape["kv"]

    def device_part(*args):
        if kernels_fit(peers, args[0], args[14], args[4], args[17]):
            return local_kernels(peers, *args)
        return local(*args)

    return jax.shard_map(
        device_part, mesh=mesh, in_specs=in_specs, out_specs=out_specs, check_vma=False
    )
```
